512 devices in a mesh: sp: 256 (over z, y, x), tp: 2 (over core).
Axes of the slice: x: 4, y: 4, z: 16, core: 2. Of those that a mesh axis runs over, the one named last changes fastest.
Arguments:
- stream: bfloat16 [1024, 131072], P('tp', 'sp'), may hold values from -6 to 6
- norm_gain: float32 [2, 1024], replicated, may hold values from 0.1 to 1.9
- w_value: bfloat16 [2, 512, 1024], P(None, 'tp'), may hold values from -0.1875 to 0.1875
- w_gate: bfloat16 [2, 512, 1024], P(None, 'tp'), may hold values from -0.1875 to 0.1875
- conv_taps: bfloat16 [2, 512, 255], P(None, 'tp'), may hold values from -0.375 to 0.375
- group_gain: float32 [2, 512], P(None, 'tp'), may hold values from 0.1 to 1.9
- group_shift: float32 [2, 512], P(None, 'tp'), may hold values from -3 to 3
- w_out: bfloat16 [2, 1024, 512], P(None, 'tp'), may hold values from -0.25 to 0.25
Outputs:
- result: bfloat16 [1024, 131072], P('tp', 'sp')
The draws below stay inside these ranges and needn't reach their ends.
All inputs are finite; a program needn't handle non-finite values.
Results may differ from the reference program's by a relative error of at most 0.014.
Values may be sent and summed in bfloat16 or wider, within the bound.
No kernel may reach another device: no remote copies, remote signals or barrier semaphores. Data moves between devices by JAX's collectives and lax.ppermute only.
A program may use at most 64 MiB of HBM per device.

```python
import math
import jax
import jax.numpy as jnp
from jax import lax

D = 1024
C = 512
GROUP_DIM = 128
KERNEL = 255
LAYERS = 2
TOK_DEV = 512
TOKENS = 131072
N_SP = 256


def shard_levels(stream_key, dims, split, least, top_value):
    def one(position, blocks):
        heights = jax.random.uniform(jax.random.fold_in(jax.random.fold_in(stream_key, 6), position), (blocks,), jnp.float32, least / len(split), top_value / len(split))
        return jnp.repeat(jnp.exp(heights), dims[position] // blocks).reshape((-1,) + (1,) * (len(dims) - position - 1))

    factor_of = one(*split[0])
    for cut in split[1:]:
        factor_of = factor_of * one(*cut)
    return factor_of


def noise(rng, extent, width, most, pieces=(), kind=jnp.bfloat16):
    level = shard_levels(rng, extent, pieces, -0.22, 0.18) if pieces else 1.0
    drawn = jax.random.normal(rng, extent, jnp.float32) * width * level
    return jnp.minimum(jnp.maximum(drawn, -most), most).astype(kind)


def setup_inputs(seed: int = 0) -> dict:
    key_list = jax.random.split(jax.random.key(seed), 9)
    return {
        "stream": noise(key_list[0], (D, TOKENS), 1.0, 6.0, ((0, 2), (1, 256))),
        "norm_gain": jnp.clip(1.0 + 0.18 * jax.random.normal(key_list[1], (LAYERS, D), jnp.float32), 0.1, 1.9),
        "w_value": noise(key_list[2], (LAYERS, C, D), D ** -0.5, 0.1875, ((1, 2),)),
        "w_gate": noise(key_list[3], (LAYERS, C, D), D ** -0.5, 0.1875, ((1, 2),)),
        "conv_taps": noise(key_list[4], (LAYERS, C, KERNEL), KERNEL ** -0.5, 0.375, ((1, 2),)),
        "group_gain": jnp.clip(1.0 + 0.18 * jax.random.normal(key_list[5], (LAYERS, C), jnp.float32), 0.1, 1.9),
        "group_shift": noise(key_list[6], (LAYERS, C), 0.5, 3.0, ((1, 2),), jnp.float32),
        "w_out": noise(key_list[7], (LAYERS, D, C), C ** -0.5, 0.25, ((1, 2),)),
    }


RMS_EPS = 1e-06
LN_EPS = 1e-05

def one_layer(stream, gain, wv, wg, taps, ggain, gshift, wo):
    rim_width = (KERNEL - 1) // 2
    total = stream.shape[1]
    block = TOK_DEV * math.gcd(N_SP, 8)
    nblocks = total // block

    def gated_block(index):
        start = (index * block).astype(jnp.int32)
        piece = lax.dynamic_slice_in_dim(stream, start, block, 1)
        widened = piece.astype(jnp.float32)
        inverse_rms = lax.rsqrt(lax.optimization_barrier(jnp.mean(widened * widened, axis=0, keepdims=True)) + RMS_EPS)
        normed = (widened * inverse_rms * gain[:, None]).astype(jnp.bfloat16)
        projected = jnp.dot(wv, normed, preferred_element_type=jnp.float32).astype(jnp.bfloat16)
        gate_proj = jnp.dot(wg, normed, preferred_element_type=jnp.float32).astype(jnp.bfloat16)
        return (projected.astype(jnp.float32) * jax.nn.sigmoid(gate_proj.astype(jnp.float32))).astype(jnp.bfloat16)
    stacked = lax.map(gated_block, jnp.arange(nblocks, dtype=jnp.int32))
    gated = jnp.moveaxis(stacked, 0, 1).reshape(C, total)
    padded = jnp.pad(gated, ((0, 0), (rim_width, rim_width)))
    taps_wide = taps.astype(jnp.float32)

    def out_block(index):
        start = (index * block).astype(jnp.int32)
        window = lax.dynamic_slice_in_dim(padded, start, block + 2 * rim_width, 1)

        def add_tap(tap, running):
            shifted = lax.dynamic_slice_in_dim(window, tap.astype(jnp.int32), block, 1)
            column = lax.dynamic_slice_in_dim(taps_wide, tap.astype(jnp.int32), 1, 1)
            return running + column * shifted.astype(jnp.float32)
        filtered = lax.fori_loop(0, KERNEL, add_tap, jnp.zeros((C, block), jnp.float32))
        grouped = filtered.reshape(C // GROUP_DIM, GROUP_DIM, block)
        group_mean = lax.optimization_barrier(jnp.mean(grouped, axis=1, keepdims=True))
        centred = grouped - group_mean
        scaled = centred * lax.rsqrt(lax.optimization_barrier(jnp.mean(centred * centred, axis=1, keepdims=True)) + LN_EPS)
        scaled = scaled.reshape(C, block) * ggain[:, None] + gshift[:, None]
        activated = jax.nn.silu(scaled).astype(jnp.bfloat16)
        branch = jnp.dot(wo, activated, preferred_element_type=jnp.float32)
        piece = lax.dynamic_slice_in_dim(stream, start, block, 1)
        return (piece.astype(jnp.float32) + branch).astype(jnp.bfloat16)
    outs = lax.map(out_block, jnp.arange(nblocks, dtype=jnp.int32))
    return jnp.moveaxis(outs, 0, 1).reshape(stream.shape[0], total)

def reference(stream, norm_gain, w_value, w_gate, conv_taps, group_gain, group_shift, w_out):
    for layer_index in range(LAYERS):
        stream = one_layer(stream, norm_gain[layer_index], w_value[layer_index], w_gate[layer_index], conv_taps[layer_index], group_gain[layer_index], group_shift[layer_index], w_out[layer_index])
    return stream
```

```python
import jax
import jax.numpy as jnp
import numpy as np
from jax import lax
from jax.sharding import PartitionSpec as P

GROUP_DIM = 128


RMS_EPS = 1e-06
LN_EPS = 1e-05

WINDOW = 512
KEPT = 256
FIRST = 128


def split_table(table):
    high = table.astype(jnp.bfloat16)
    low = (table - high.astype(np.float64)).astype(jnp.bfloat16)
    return high, low


def transform_tables(taps):
    bins = 2 * np.arange(WINDOW // 2) + 1
    reach = (taps - 1) // 2

    def angles(left, right):
        return np.pi * (np.outer(left, right) % (2 * WINDOW)) / WINDOW

    time = angles(np.arange(WINDOW), bins)
    forward = np.concatenate([np.cos(time), -np.sin(time)], 1)
    lag = angles(np.arange(taps) - reach, bins)
    tap_side = np.concatenate([np.cos(lag), np.sin(lag)], 1) * (2.0 / WINDOW)
    back = angles(bins, np.arange(FIRST, FIRST + KEPT))
    inverse = np.concatenate([np.cos(back), -np.sin(back)], 0)
    fh, fl = split_table(forward)
    th, tl = split_table(tap_side)
    ih, il = split_table(inverse)
    return (
        np.concatenate([fh, fl], 0),
        np.concatenate([th, tl], 0),
        np.concatenate([ih, ih, il], 0),
    )


def gathered(value, dim):
    return lax.all_gather(value, "tp", axis=dim, tiled=True)


def dot(a, b):
    return jnp.dot(a, b, preferred_element_type=jnp.float32)


def with_halo(cells, width):
    count = lax.axis_size("sp")
    ends = count - 1
    head = cells[:, :width]
    tail = cells[:, cells.shape[1] - width :]
    return jnp.concatenate(
        [
            lax.ppermute(tail, "sp", [(i, i + 1) for i in range(ends)]),
            cells,
            lax.ppermute(head, "sp", [(i + 1, i) for i in range(ends)]),
        ],
        axis=1,
    )


def make_gated(whole, gain, value_weight, gate_weight):
    widened = whole.astype(jnp.float32)
    inverse_rms = lax.rsqrt(jnp.mean(widened * widened, axis=0, keepdims=True) + RMS_EPS)
    normed = (widened * inverse_rms * gain[:, None]).astype(jnp.bfloat16)
    projected = dot(value_weight, normed).astype(jnp.bfloat16)
    gate_proj = dot(gate_weight, normed).astype(jnp.bfloat16)
    return (projected.astype(jnp.float32) * jax.nn.sigmoid(gate_proj.astype(jnp.float32))).astype(
        jnp.bfloat16
    )


def filter_norm(padded, tap_bins, tables, ggain, gshift):
    channels = padded.shape[0]
    half = WINDOW // 2
    tap_re, tap_im = tap_bins[:, :half], tap_bins[:, half:]
    kept = []
    for start in range(0, padded.shape[1] - KEPT, KEPT):
        piece = padded[:, start : start + WINDOW]
        freq = dot(jnp.concatenate([piece, piece], 1), tables[0])
        re, im = freq[:, :half], freq[:, half:]
        prod = jnp.concatenate([re * tap_re - im * tap_im, re * tap_im + im * tap_re], 1)
        high = prod.astype(jnp.bfloat16)
        low = (prod - high.astype(jnp.float32)).astype(jnp.bfloat16)
        kept.append(dot(jnp.concatenate([high, low, high], 1), tables[2]))
    filtered = jnp.concatenate(kept, 1)
    tokens_here = filtered.shape[1]
    grouped = filtered.reshape(channels // GROUP_DIM, GROUP_DIM, tokens_here)
    group_mean = jnp.mean(grouped, axis=1, keepdims=True)
    centred = grouped - group_mean
    scaled = centred * lax.rsqrt(jnp.mean(centred * centred, axis=1, keepdims=True) + LN_EPS)
    scaled = scaled.reshape(channels, tokens_here) * ggain[:, None] + gshift[:, None]
    return jax.nn.silu(scaled).astype(jnp.bfloat16)


def body(stream, norm_gain, w_value, w_gate, conv_taps, group_gain, group_shift, w_out):
    taps = conv_taps.shape[2]
    layers = w_value.shape[0]
    tables = transform_tables(taps)
    for layer_index in range(layers):
        part = stream.shape[0] // 2
        tokens = stream.shape[1]
        low_rows = lax.all_gather(stream[:part], "tp", axis=0)
        high_rows = lax.all_gather(stream[part:], "tp", axis=0)
        whole = jnp.stack([low_rows, high_rows], 1).reshape(-1, tokens)
        gated = make_gated(whole, norm_gain[layer_index], w_value[layer_index], w_gate[layer_index])
        padded = with_halo(gated, 128)
        both = jnp.concatenate([conv_taps[layer_index]] * 2, 1)
        tap_bins = dot(both, tables[1])
        activated = filter_norm(
            padded, tap_bins, tables, group_gain[layer_index], group_shift[layer_index]
        )
        branch = dot(w_out[layer_index], gathered(activated, 0))
        stream = (stream.astype(jnp.float32) + branch).astype(jnp.bfloat16)
    return stream


def solution(mesh):
    placed = (
        P("tp", "sp"),
        P(),
        P(None, "tp", None),
        P(None, "tp", None),
        P(None, "tp", None),
        P(None, "tp"),
        P(None, "tp"),
        P(None, "tp", None),
    )
    return jax.shard_map(body, mesh=mesh, in_specs=placed, out_specs=P("tp", "sp"), check_vma=False)
```

```python
import functools

import jax
import jax.numpy as jnp
import numpy as np
from jax import lax
from jax.experimental import pallas as pl
from jax.experimental.pallas import tpu as pltpu
from jax.sharding import PartitionSpec as P


RMS_EPS = 1e-06
LN_EPS = 1e-05

WINDOW = 512
KEPT = 256
FIRST = 128
BINS = WINDOW // 2
TAP_ROW = 1536
GAIN_ROW = 1664
PACK_ROWS = 1680
HALF = 256


def transform_tables(taps):
    bins = 2 * np.arange(BINS) + 1
    reach = (taps - 1) // 2

    def angles(left, right):
        return np.pi * (np.outer(left, right) % (2 * WINDOW)) / WINDOW

    time = angles(np.arange(WINDOW), bins)
    lag = angles(np.arange(taps) - reach, bins)
    back = angles(bins, np.arange(FIRST, FIRST + KEPT))
    tap_side = np.concatenate([np.cos(lag), np.sin(lag)], 1) * (2.0 / WINDOW)
    tap_side = np.pad(tap_side, ((0, 256 - taps), (0, 0)))
    forward = np.concatenate([np.cos(time), -np.sin(time)], 1)
    inverse = np.concatenate([np.cos(back), -np.sin(back)], 0)

    def terms(table):
        high = table.astype(jnp.bfloat16)
        return high, (table - high.astype(np.float64)).astype(jnp.bfloat16)

    return np.concatenate(
        [*terms(tap_side), *terms(forward), np.concatenate(terms(inverse), 1)], 0
    )


def dot(a, b):
    return jnp.dot(a, b, preferred_element_type=jnp.float32)


def column(row):
    return jnp.transpose(jnp.broadcast_to(row, (128, 128)))


def wide(col):
    return jnp.concatenate([col, col], 1)


def sigmoid(value):
    return 0.5 * jnp.tanh(0.5 * value) + 0.5


def layers_kernel(
    place, own, near, far, halo, gain, pack, pack2, tables, keep, send,
    xw, normed, gated, act, x1, gated2, act2, bins, gains, gcols, table, sems,
):
    me = place[0]
    other = 1 - me
    packs = (pack, pack2)

    copies = [
        pltpu.make_async_copy(
            tables.at[pl.ds(start, size)], table.at[pl.ds(start, size)], sems.at[i]
        )
        for i, (start, size) in enumerate(((0, 512), (512, 1024), (1536, 512)))
    ]
    for copy in copies:
        copy.start()

    def lanes(block, size=HALF):
        return pl.ds(pl.multiple_of(block * size, size), size)

    first = other
    for part in range(2):
        xw[:512, lanes(first + part)] = own[:, part * HALF : (part + 1) * HALF]
    xw[512:, lanes(first + me)] = near[other]
    xw[512:, lanes(first + other)] = far[other]
    xw[512:, lanes(2 * me)] = halo[:512]
    xw[:512, lanes(2 * me)] = halo[512:]

    for layer in range(2):
        for half, block in enumerate((me, other)):
            for j in range(4):
                row = gain[layer : layer + 1, lanes(4 * block + j, 128)]
                start = half * 512 + j * 128
                gains[layer, start : start + 128] = column(row)
        for chunk, source in enumerate(packs):
            terms = source[GAIN_ROW : GAIN_ROW + 16, :256].astype(jnp.float32)
            for g in range(2):
                for kind in range(2):
                    t = terms[:, g * 128 : (g + 1) * 128]
                    i = 6 * layer + 3 * kind
                    row = t[i : i + 1] + t[i + 1 : i + 2] + t[i + 2 : i + 3]
                    start = chunk * 256 + g * 128
                    gcols[layer, kind, start : start + 128] = column(row)

    def norm(source, tile, layer, slot):
        cols = slice(tile * HALF, (tile + 1) * HALF)
        total = jnp.zeros((8, HALF), jnp.float32)
        for r in range(0, 1024, 128):
            piece = source[r : r + 128, cols].astype(jnp.float32)
            square = piece * piece
            for s in range(0, 128, 8):
                total += square[s : s + 8]
        mean = jnp.sum(total, axis=0, keepdims=True) * (1.0 / 1024.0)
        inverse = lax.rsqrt(mean + RMS_EPS)
        for j in range(8):
            r = slice(j * 128, (j + 1) * 128)
            piece = source[r, cols].astype(jnp.float32)
            normed[slot, r, :] = (piece * inverse * wide(gains[layer, r])).astype(jnp.bfloat16)

    def project(slot, layer, target, tile):
        cols = slice(tile * HALF, (tile + 1) * HALF)
        for chunk, source in enumerate(packs):
            def product(start):
                r = slice(start + layer * 256, start + (layer + 1) * 256)
                total = dot(source[r, lanes(me, 512)], normed[slot, :512])
                return total + dot(source[r, lanes(other, 512)], normed[slot, 512:])

            projected = product(0).astype(jnp.bfloat16).astype(jnp.float32)
            gate_proj = product(512).astype(jnp.bfloat16).astype(jnp.float32)
            target[chunk * 256 : (chunk + 1) * 256, cols] = (
                projected * sigmoid(gate_proj)
            ).astype(jnp.bfloat16)

    def make_bins(layer):
        for chunk, source in enumerate(packs):
            for part in range(2):
                lane = (2 * layer + part) * 256
                taps = source[TAP_ROW : TAP_ROW + 128, lane : lane + 256]
                start = chunk * 256 + part * 128
                bins[layer, start : start + 128] = dot(taps, table[:256]) + dot(
                    taps, table[256:512]
                )

    def filter_norm(source, start, layer, target):
        for chunk in range(2):
            r = slice(chunk * 256, (chunk + 1) * 256)
            piece = source[r, start : start + WINDOW]
            freq = dot(piece, table[512:1024]) + dot(piece, table[1024:1536])
            re, im = freq[:, :BINS], freq[:, BINS:]
            tap_re, tap_im = bins[layer, r, :BINS], bins[layer, r, BINS:]
            prod = jnp.concatenate(
                [re * tap_re - im * tap_im, re * tap_im + im * tap_re], 1
            )
            high = prod.astype(jnp.bfloat16)
            low = (prod - high.astype(jnp.float32)).astype(jnp.bfloat16)
            ih, il = table[1536:2048, :KEPT], table[1536:2048, KEPT:]
            filtered = dot(high, ih) + dot(low, ih) + dot(high, il)
            for g in range(2):
                v = filtered[g * 128 : (g + 1) * 128]
                c = slice(chunk * 256 + g * 128, chunk * 256 + (g + 1) * 128)
                centred = v - jnp.mean(v, axis=0, keepdims=True)
                var = jnp.mean(centred * centred, axis=0, keepdims=True)
                scaled = centred * lax.rsqrt(var + LN_EPS)
                scaled = scaled * wide(gcols[layer, 0, c]) + wide(gcols[layer, 1, c])
                target[c, :] = (scaled * sigmoid(scaled)).astype(jnp.bfloat16)

    def branch(source, layer, activated):
        r = slice(1024, 1536)
        total = dot(source[r, lanes(2 * layer + me)], activated[:256])
        return total + dot(source[r, lanes(2 * layer + other)], activated[256:])

    lane = lax.broadcasted_iota(jnp.int32, (8, KEPT), 1)
    outside = (
        (lane < FIRST) & (place[1] == 1),
        (lane >= KEPT - FIRST) & (place[2] == 1),
    )

    def finish_first(b):
        cols = slice(FIRST + b * KEPT, FIRST + (b + 1) * KEPT)
        for half, source in enumerate(packs):
            r = slice(half * 512, (half + 1) * 512)
            total = xw[r, cols].astype(jnp.float32) + branch(source, 0, act[b])
            drop = jnp.broadcast_to(outside[b][:1], total.shape)
            total = jnp.where(drop, 0.0, total)
            x1[r, b * KEPT : (b + 1) * KEPT] = total.astype(jnp.bfloat16)

    norm(xw, 0, 0, 0)
    norm(xw, 1, 0, 1)
    copies[0].wait()
    make_bins(0)
    project(0, 0, gated, 0)
    norm(xw, 2, 0, 2)
    project(1, 0, gated, 1)
    copies[1].wait()
    copies[2].wait()
    filter_norm(gated, 0, 0, act.at[0])
    project(2, 0, gated, 2)
    finish_first(0)
    filter_norm(gated, KEPT, 0, act.at[1])
    norm(x1, 0, 1, 3)
    finish_first(1)
    make_bins(1)
    project(3, 1, gated2, 0)
    norm(x1, 1, 1, 4)
    project(4, 1, gated2, 1)
    filter_norm(gated2, 0, 1, act2)
    cols = slice(FIRST, FIRST + KEPT)
    for half, (source, out) in enumerate(((pack, keep), (pack2, send))):
        before = x1[half * 512 : (half + 1) * 512, cols].astype(jnp.float32)
        out[...] = (before + branch(source, 1, act2)).astype(jnp.bfloat16)


def run_layers(place, arrays):
    vmem = pl.BlockSpec(memory_space=pltpu.VMEM)
    out = jax.ShapeDtypeStruct((512, KEPT), jnp.bfloat16)
    return pl.pallas_call(
        layers_kernel,
        out_shape=[out, out],
        in_specs=[pl.BlockSpec(memory_space=pltpu.SMEM)]
        + [vmem] * (len(arrays) - 1)
        + [pl.BlockSpec(memory_space=pltpu.HBM)],
        out_specs=[vmem, vmem],
        scratch_shapes=[
            pltpu.VMEM((1024, 768), jnp.bfloat16),
            pltpu.VMEM((5, 1024, HALF), jnp.bfloat16),
            pltpu.VMEM((512, 768), jnp.bfloat16),
            pltpu.VMEM((2, 512, KEPT), jnp.bfloat16),
            pltpu.VMEM((1024, 512), jnp.bfloat16),
            pltpu.VMEM((512, 512), jnp.bfloat16),
            pltpu.VMEM((512, KEPT), jnp.bfloat16),
            pltpu.VMEM((2, 512, WINDOW), jnp.float32),
            pltpu.VMEM((2, 1024, 128), jnp.float32),
            pltpu.VMEM((2, 2, 512, 128), jnp.float32),
            pltpu.VMEM((2048, 512), jnp.bfloat16),
            pltpu.SemaphoreType.DMA((3,)),
        ],
        compiler_params=pltpu.CompilerParams(vmem_limit_bytes=28 << 20),
        cost_estimate=pl.CostEstimate(
            flops=7 * 10**9, bytes_accessed=10**7, transcendentals=2 * 10**6
        ),
    )(place, *arrays)


def pack_kernel(after, wv, wg, wo, taps0, taps1, ggain, gshift, out, sems):
    copies = []
    for layer in range(2):
        for start, source in ((0, wv), (512, wg)):
            copies.append((source.at[layer], out.at[pl.ds(start + layer * 256, 256)]))
        copies.append((wo.at[layer], out.at[pl.ds(1024, 512), pl.ds(512 * layer, 512)]))
    copies = [
        pltpu.make_async_copy(source, target, sems.at[i])
        for i, (source, target) in enumerate(copies)
    ]
    for copy in copies:
        copy.start()
    for layer, taps in enumerate((taps0, taps1)):
        for chunk in range(2):
            lane = (2 * layer + chunk) * 256
            piece = jnp.pad(taps[chunk * 128 : (chunk + 1) * 128], ((0, 0), (0, 1)))
            out[TAP_ROW : TAP_ROW + 128, lane : lane + 256] = piece
    rows = []
    for layer in range(2):
        for source in (ggain, gshift):
            rest = source[layer : layer + 1]
            for _ in range(3):
                term = rest.astype(jnp.bfloat16).astype(jnp.float32)
                rows.append(term)
                rest = rest - term
    rows.append(jnp.zeros((4, 256), jnp.float32))
    rows = jnp.concatenate(rows, 0).astype(jnp.bfloat16)
    out[GAIN_ROW:PACK_ROWS, :] = jnp.concatenate([rows, rows, rows, rows], 1)
    for copy in copies:
        copy.wait()


def run_pack(after, wv, wg, wo, taps, ggain, gshift):
    vmem = pl.BlockSpec(memory_space=pltpu.VMEM)
    anywhere = pl.BlockSpec(memory_space=pltpu.HBM)
    after_spec = pl.BlockSpec(memory_space=pl.ANY)
    return pl.pallas_call(
        pack_kernel,
        out_shape=jax.ShapeDtypeStruct((PACK_ROWS, 1024), jnp.bfloat16),
        in_specs=[after_spec] + [anywhere] * 3 + [vmem] * 4,
        out_specs=vmem,
        scratch_shapes=[pltpu.SemaphoreType.DMA((6,))],
        compiler_params=pltpu.CompilerParams(vmem_limit_bytes=8 << 20),
        cost_estimate=pl.CostEstimate(
            flops=2 * 10**9, bytes_accessed=7 * 10**6, transcendentals=0
        ),
    )(after, wv, wg, wo, taps[0], taps[1], ggain, gshift)


def body(blocks, stream, norm_gain, w_value, w_gate, conv_taps, group_gain, group_shift, w_out):
    taps = conv_taps.shape[2]
    me = lax.axis_index("tp")
    block = lax.axis_index("sp")
    both = ("sp", "tp")
    partner = [(i, i ^ 1) for i in range(2 * blocks)]
    outward = [(2 * s + 1, 2 * s + 2) for s in range(blocks - 1)]
    outward += [(2 * s + 2, 2 * s + 1) for s in range(blocks - 1)]

    outer = lax.dynamic_slice_in_dim(stream, HALF * me, HALF, 1)
    inner = lax.dynamic_slice_in_dim(stream, HALF * (1 - me), HALF, 1)
    near = lax.all_gather(inner, "tp", axis=0)
    mine = jnp.concatenate([outer, lax.dynamic_index_in_dim(near, 1 - me, 0, False)], 0)
    tables = jnp.asarray(transform_tables(taps))
    mine, conv_taps = lax.optimization_barrier((mine, conv_taps))
    halo = lax.ppermute(mine, both, outward)
    pack = run_pack(mine, w_value, w_gate, w_out, conv_taps, group_gain, group_shift)
    pack2 = lax.ppermute(pack, both, partner)
    far = lax.all_gather(outer, "tp", axis=0)

    place = jnp.stack(
        [me, (me == 0) & (block == 0), (me == 1) & (block == blocks - 1)]
    ).astype(jnp.int32)
    keep, send = run_layers(
        place,
        [stream, near, far, halo, norm_gain, pack, pack2, tables],
    )
    swapped = lax.all_gather(send, "tp", axis=0)
    return jnp.concatenate(
        [jnp.where(me == 0, keep, swapped[0]), jnp.where(me == 0, swapped[1], keep)], 1
    )


def solution(mesh):
    placed = (
        P("tp", "sp"),
        P(),
        P(None, "tp", None),
        P(None, "tp", None),
        P(None, "tp", None),
        P(None, "tp"),
        P(None, "tp"),
        P(None, "tp", None),
    )
    return jax.shard_map(
        functools.partial(body, mesh.shape["sp"]),
        mesh=mesh, in_specs=placed, out_specs=P("tp", "sp"), check_vma=False,
    )
```

```python
import functools

import jax
import jax.numpy as jnp
import numpy as np
from jax import lax
from jax.experimental import pallas as pl
from jax.experimental.pallas import tpu as pltpu
from jax.sharding import PartitionSpec as P


RMS_EPS = 1e-06
LN_EPS = 1e-05

WINDOW = 512
KEPT = 256
FIRST = 128
BINS = WINDOW // 2
HALF = 256
GATE_ROW = 256
OUT_ROW = 512
TAP_ROW = 768
GAIN_ROW = 896
OUTER_ROW = 912


def transform_tables(taps):
    bins = 2 * np.arange(BINS) + 1
    reach = (taps - 1) // 2

    def angles(left, right):
        return np.pi * (np.outer(left, right) % (2 * WINDOW)) / WINDOW

    time = angles(np.arange(WINDOW), bins)
    lag = angles(np.arange(taps) - reach, bins)
    back = angles(bins, np.arange(FIRST, FIRST + KEPT))
    tap_side = np.concatenate([np.cos(lag), np.sin(lag)], 1) * (2.0 / WINDOW)
    tap_side = np.pad(tap_side, ((0, 256 - taps), (0, 0)))
    forward = np.concatenate([np.cos(time), -np.sin(time)], 1)
    inverse = np.concatenate([np.cos(back), -np.sin(back)], 0)

    def terms(table):
        high = table.astype(jnp.bfloat16)
        return high, (table - high.astype(np.float64)).astype(jnp.bfloat16)

    return np.concatenate(
        [*terms(tap_side), *terms(forward), np.concatenate(terms(inverse), 1)], 0
    )


def dot(a, b):
    return jnp.dot(a, b, preferred_element_type=jnp.float32)


def column(row):
    return jnp.transpose(jnp.broadcast_to(row, (128, 128)))


def wide(col):
    return jnp.concatenate([col, col], 1)


def sigmoid(value):
    return 0.5 * jnp.tanh(0.5 * value) + 0.5


def lanes(block, size=HALF):
    return pl.ds(pl.multiple_of(block * size, size), size)


def norm_tile(source, cols, gains, layer, store):
    total = jnp.zeros((8, HALF), jnp.float32)
    for r in range(0, 1024, 128):
        piece = source[r : r + 128, cols].astype(jnp.float32)
        square = piece * piece
        for s in range(0, 128, 8):
            total += square[s : s + 8]
    mean = jnp.sum(total, axis=0, keepdims=True) * (1.0 / 1024.0)
    inverse = lax.rsqrt(mean + RMS_EPS)
    for j in range(8):
        r = slice(j * 128, (j + 1) * 128)
        piece = source[r, cols].astype(jnp.float32)
        store[r, :] = (piece * inverse * wide(gains[layer, r])).astype(jnp.bfloat16)


def project_tile(source, tokens, me):
    def product(start):
        r = slice(start, start + 256)
        total = dot(source[r, lanes(me, 512)], tokens[:512])
        total = total + dot(source[r, lanes(1 - me, 512)], tokens[512:])
        return total.astype(jnp.bfloat16).astype(jnp.float32)

    return (product(0) * sigmoid(product(GATE_ROW))).astype(jnp.bfloat16)


def branch(source, half, activated, me):
    r = slice(OUT_ROW, OUT_ROW + 256)
    total = dot(source[r, lanes(2 * half + me)], activated[:256])
    return total + dot(source[r, lanes(2 * half + 1 - me)], activated[256:])


def make_bins(source, layer, part, table):
    lane = (2 * layer + part) * 256
    taps = source[TAP_ROW : TAP_ROW + 128, lane : lane + 256]
    return dot(taps, table[:256]) + dot(taps, table[256:512])


def filter_norm(piece_of, bins, gcols, table, target):
    for chunk in range(2):
        piece = piece_of(slice(chunk * 256, (chunk + 1) * 256))
        freq = dot(piece, table[512:1024]) + dot(piece, table[1024:1536])
        re, im = freq[:, :BINS], freq[:, BINS:]
        tap_re, tap_im = bins[chunk][:, :BINS], bins[chunk][:, BINS:]
        prod = jnp.concatenate([re * tap_re - im * tap_im, re * tap_im + im * tap_re], 1)
        high = prod.astype(jnp.bfloat16)
        low = (prod - high.astype(jnp.float32)).astype(jnp.bfloat16)
        ih, il = table[1536:2048, :KEPT], table[1536:2048, KEPT:]
        filtered = dot(high, ih) + dot(low, ih) + dot(high, il)
        for g in range(2):
            v = filtered[g * 128 : (g + 1) * 128]
            c = slice(chunk * 256 + g * 128, chunk * 256 + (g + 1) * 128)
            centred = v - jnp.mean(v, axis=0, keepdims=True)
            var = jnp.mean(centred * centred, axis=0, keepdims=True)
            scaled = centred * lax.rsqrt(var + LN_EPS)
            scaled = scaled * wide(gcols[0, c]) + wide(gcols[1, c])
            target[c, :] = (scaled * sigmoid(scaled)).astype(jnp.bfloat16)


def group_columns(packs, layer, gcols):
    for chunk, source in enumerate(packs):
        terms = source[GAIN_ROW : GAIN_ROW + 16, :256].astype(jnp.float32)
        for g in range(2):
            for kind in range(2):
                t = terms[:, g * 128 : (g + 1) * 128]
                i = 6 * layer + 3 * kind
                row = t[i : i + 1] + t[i + 1 : i + 2] + t[i + 2 : i + 3]
                start = chunk * 256 + g * 128
                gcols[kind, start : start + 128] = column(row)


def early_kernel(tokens, gain, pack, table, normed, gated, bins, gains):
    me = lax.axis_index("tp")
    other = 1 - me
    for layer in range(2):
        for half, side in enumerate((me, other)):
            for j in range(4):
                row = gain[layer : layer + 1, lanes(4 * side + j, 128)]
                start = half * 512 + j * 128
                gains[layer, start : start + 128] = column(row)
    norm_tile(tokens, slice(0, HALF), gains, 0, normed)
    for layer in range(2):
        for part in range(2):
            bins[layer, part * 128 : (part + 1) * 128] = make_bins(pack, layer, part, table)
    gated[...] = project_tile(pack, normed, me)


def first_kernel(
    tokens, normed, gated_own, bins, gains, inner, halo, pack, pack2, table, x1, normed2,
    xw, normed1, gated, act, bins2, gcols,
):
    me = lax.axis_index("tp")
    block = lax.axis_index("sp")
    other = 1 - me
    packs = (pack, pack2)

    def stored(tile):
        return lanes(tile * me + (2 - tile) * other)

    xw[:512, :256] = inner[...]
    for q in range(4):
        r = slice(512 + 128 * q, 512 + 128 * (q + 1))
        xw[r, :256] = pack2[OUTER_ROW : OUTER_ROW + 128, 256 * q : 256 * (q + 1)]
    xw[:512, 512:] = halo[512:]
    xw[512:, 512:] = halo[:512]
    xw[:, 256:512] = tokens[...]
    for slot, tile in enumerate((0, 2)):
        cols = slice(tile * HALF, (tile + 1) * HALF)
        norm_tile(xw, cols, gains, 0, normed1.at[slot])
    group_columns(packs, 0, gcols)
    for part in range(2):
        bins2[part * 128 : (part + 1) * 128] = make_bins(pack2, 0, part, table)
    gated[:256, 256:512] = gated_own[...]
    gated[256:, 256:512] = project_tile(pack2, normed, me)
    for slot, tile in enumerate((0, 2)):
        cols = slice(tile * HALF, (tile + 1) * HALF)
        for chunk, source in enumerate(packs):
            r = slice(chunk * 256, (chunk + 1) * 256)
            gated[r, cols] = project_tile(source, normed1.at[slot], me)

    lane = lax.broadcasted_iota(jnp.int32, (8, KEPT), 1)
    ends = lax.axis_size("sp") - 1
    outside = (
        (lane < FIRST) & ((me == 0) & (block == 0)),
        (lane >= KEPT - FIRST) & ((me == 1) & (block == ends)),
    )

    def piece(b):
        return lambda r: jnp.concatenate([gated[r, stored(b)], gated[r, stored(b + 1)]], 1)

    def finish(b):
        for half, source in enumerate(packs):
            for part in range(2):
                start = half * 512 + part * 256
                r = slice(start, start + 256)
                before = jnp.concatenate(
                    [xw[r, stored(b)][:, FIRST:], xw[r, stored(b + 1)][:, :FIRST]], 1
                )
                total = before.astype(jnp.float32) + branch(source, part, act[b], me)
                drop = jnp.broadcast_to(outside[b][:1], total.shape)
                total = jnp.where(drop, 0.0, total)
                x1[r, b * KEPT : (b + 1) * KEPT] = total.astype(jnp.bfloat16)

    own = bins[0], bins2[...]
    filter_norm(piece(0), own, gcols, table, act.at[0])
    finish(0)
    filter_norm(piece(1), own, gcols, table, act.at[1])
    norm_tile(x1, slice(0, 256), gains, 1, normed2.at[0])
    finish(1)
    norm_tile(x1, slice(256, 512), gains, 1, normed2.at[1])


def second_kernel(
    x1, normed2, bins, pack, pack2, late, late2, table, keep, send, gated, act, bins2, gcols
):
    me = lax.axis_index("tp")
    group_columns((pack, pack2), 1, gcols)
    for part in range(2):
        bins2[part * 128 : (part + 1) * 128] = make_bins(pack2, 1, part, table)
    for tile in range(2):
        for chunk, source in enumerate((late, late2)):
            r = slice(chunk * 256, (chunk + 1) * 256)
            cols = slice(tile * HALF, (tile + 1) * HALF)
            gated[r, cols] = project_tile(source, normed2.at[tile], me)
    filter_norm(lambda r: gated[r, :], (bins[1], bins2[...]), gcols, table, act)
    cols = slice(FIRST, FIRST + KEPT)
    for half, (source, out) in enumerate(((late, keep), (late2, send))):
        for part in range(2):
            start = half * 512 + part * 256
            before = x1[start : start + 256, cols].astype(jnp.float32)
            total = before + branch(source, part, act, me)
            out[part * 256 : (part + 1) * 256] = total.astype(jnp.bfloat16)


def weight_copies(layer, wv, wg, wo, out, sems):
    copies = [
        (wv.at[layer], out.at[pl.ds(0, 256)]),
        (wg.at[layer], out.at[pl.ds(GATE_ROW, 256)]),
    ]
    for part in range(2):
        rows = pl.ds(256 * part, 256)
        copies.append((wo.at[layer, rows], out.at[pl.ds(OUT_ROW, 256), pl.ds(512 * part, 512)]))
    copies = [pltpu.make_async_copy(a, b, sems.at[i]) for i, (a, b) in enumerate(copies)]
    for copy in copies:
        copy.start()
    return copies


def pack_kernel(after, wv, wg, wo, taps0, taps1, ggain, gshift, outer, out, turned, sems):
    copies = weight_copies(0, wv, wg, wo, out, sems)
    for layer, taps in enumerate((taps0, taps1)):
        count = taps.shape[0]
        turned[:count] = taps[...].astype(jnp.float32)
        turned[count:] = jnp.zeros((256 - count, 256), jnp.float32)
        piece = jnp.transpose(turned[...]).astype(jnp.bfloat16)
        for chunk in range(2):
            lane = (2 * layer + chunk) * 256
            out[TAP_ROW : TAP_ROW + 128, lane : lane + 256] = piece[
                chunk * 128 : (chunk + 1) * 128
            ]
    for q in range(4):
        out[OUTER_ROW : OUTER_ROW + 128, 256 * q : 256 * (q + 1)] = outer[
            128 * q : 128 * (q + 1)
        ]
    rows = []
    for layer in range(2):
        for source in (ggain, gshift):
            rest = source[layer : layer + 1]
            for _ in range(3):
                term = rest.astype(jnp.bfloat16).astype(jnp.float32)
                rows.append(term)
                rest = rest - term
    rows.append(jnp.zeros((4, 256), jnp.float32))
    rows = jnp.concatenate(rows, 0).astype(jnp.bfloat16)
    out[GAIN_ROW:OUTER_ROW, :] = jnp.concatenate([rows, rows, rows, rows], 1)
    for copy in copies:
        copy.wait()


def late_pack_kernel(after, wv, wg, wo, out, sems):
    for copy in weight_copies(1, wv, wg, wo, out, sems):
        copy.wait()


def call(kernel, arrays, outs, scratch, limit, flops, unread=0, hbm=0):
    vmem = pl.BlockSpec(memory_space=pltpu.VMEM)
    specs = [pl.BlockSpec(memory_space=pl.ANY)] * unread
    specs += [pl.BlockSpec(memory_space=pltpu.HBM)] * hbm
    specs += [vmem] * (len(arrays) - unread - hbm)
    outs = [jax.ShapeDtypeStruct(shape, kind) for shape, kind in outs]
    return pl.pallas_call(
        kernel,
        out_shape=outs,
        in_specs=specs,
        out_specs=[vmem] * len(outs),
        scratch_shapes=scratch,
        compiler_params=pltpu.CompilerParams(vmem_limit_bytes=limit << 20),
        cost_estimate=pl.CostEstimate(
            flops=flops, bytes_accessed=4 * 10**6, transcendentals=2 * 10**5
        ),
    )(*arrays)


def body(blocks, stream, norm_gain, w_value, w_gate, conv_taps, group_gain, group_shift, w_out):
    taps = conv_taps.shape[2]
    me = lax.axis_index("tp")
    both = ("sp", "tp")
    partner = [(i, i ^ 1) for i in range(2 * blocks)]
    outward = [(2 * s + 1, 2 * s + 2) for s in range(blocks - 1)]
    outward += [(2 * s + 2, 2 * s + 1) for s in range(blocks - 1)]

    bf16, f32 = jnp.bfloat16, jnp.float32
    is_first = me == 0
    head, tail = stream[:, :HALF], stream[:, HALF:]
    outer = jnp.where(is_first, head, tail)
    inner = jnp.where(is_first, tail, head)
    inner, is_first = lax.optimization_barrier((inner, is_first))
    near = lax.all_gather(inner, "tp", axis=0)
    mine = jnp.concatenate([outer, jnp.where(is_first, near[1], near[0])], 0)
    tables = jnp.asarray(transform_tables(taps))
    mine, conv_taps = lax.optimization_barrier((mine, conv_taps))
    weights = [w_value, w_gate, w_out]
    halo = lax.ppermute(mine, both, outward)
    turned = [jnp.transpose(conv_taps[layer]) for layer in range(2)]
    (pack,) = call(
        pack_kernel,
        [mine, *weights, *turned, group_gain, group_shift, outer],
        [((OUTER_ROW + 128, 1024), bf16)],
        [pltpu.VMEM((256, 256), f32), pltpu.SemaphoreType.DMA((4,))],
        8, 2 * 10**9, 1, 3,
    )
    pack2 = lax.ppermute(pack, both, partner)
    (late,) = call(
        late_pack_kernel, [pack, *weights], [((TAP_ROW, 1024), bf16)],
        [pltpu.SemaphoreType.DMA((4,))], 4, 10**9, 1, 3,
    )
    late2 = lax.ppermute(late, both, partner)
    normed, gated, bins, gains = call(
        early_kernel,
        [mine, norm_gain, pack, tables],
        [
            ((1024, HALF), bf16), ((256, HALF), bf16),
            ((2, 256, WINDOW), f32), ((2, 1024, 128), f32),
        ],
        [], 12, 10**9,
    )
    x1, normed2 = call(
        first_kernel,
        [mine, normed, gated, bins, gains, inner, halo, pack, pack2, tables],
        [((1024, 512), bf16), ((2, 1024, HALF), bf16)],
        [
            pltpu.VMEM((1024, 768), bf16),
            pltpu.VMEM((2, 1024, HALF), bf16),
            pltpu.VMEM((512, 768), bf16),
            pltpu.VMEM((2, 512, KEPT), bf16),
            pltpu.VMEM((256, WINDOW), f32),
            pltpu.VMEM((2, 512, 128), f32),
        ],
        16, 4 * 10**9,
    )
    keep, send = call(
        second_kernel,
        [x1, normed2, bins, pack, pack2, late, late2, tables],
        [((512, KEPT), bf16), ((512, KEPT), bf16)],
        [
            pltpu.VMEM((512, 512), bf16),
            pltpu.VMEM((512, KEPT), bf16),
            pltpu.VMEM((256, WINDOW), f32),
            pltpu.VMEM((2, 512, 128), f32),
        ],
        12, 3 * 10**9,
    )
    swapped = lax.all_gather(send, "tp", axis=0)
    return jnp.concatenate(
        [jnp.where(is_first, keep, swapped[0]), jnp.where(is_first, swapped[1], keep)], 1
    )


def solution(mesh):
    placed = (
        P("tp", "sp"),
        P(),
        P(None, "tp", None),
        P(None, "tp", None),
        P(None, "tp", None),
        P(None, "tp"),
        P(None, "tp"),
        P(None, "tp", None),
    )
    return jax.shard_map(
        functools.partial(body, mesh.shape["sp"]),
        mesh=mesh, in_specs=placed, out_specs=P("tp", "sp"), check_vma=False,
    )
```

```python
import functools

import jax
import jax.numpy as jnp
import numpy as np
from jax import lax
from jax.experimental import pallas as pl
from jax.experimental.pallas import tpu as pltpu
from jax.sharding import PartitionSpec as P


RMS_EPS = 1e-06
LN_EPS = 1e-05

WINDOW = 512
KEPT = 256
FIRST = 128
BINS = WINDOW // 2
HALF = 256
GATE_ROW = 256
TAP_ROW = 512
GAIN_ROW = 640
TOKEN_ROW = 656
PACK_ROWS = 912
OUT_ROW = 512
LATE_ROWS = 1024


def transform_tables(taps):
    bins = 2 * np.arange(BINS) + 1
    reach = (taps - 1) // 2

    def angles(left, right):
        return np.pi * (np.outer(left, right) % (2 * WINDOW)) / WINDOW

    time = angles(np.arange(WINDOW), bins)
    lag = angles(np.arange(taps) - reach, bins)
    back = angles(bins, np.arange(FIRST, FIRST + KEPT))
    tap_side = np.concatenate([np.cos(lag), np.sin(lag)], 1) * (2.0 / WINDOW)
    tap_side = np.pad(tap_side, ((0, 256 - taps), (0, 0)))
    forward = np.concatenate([np.cos(time), -np.sin(time)], 1)
    inverse = np.concatenate([np.cos(back), -np.sin(back)], 0)

    def terms(table):
        high = table.astype(jnp.bfloat16)
        return high, (table - high.astype(np.float64)).astype(jnp.bfloat16)

    return np.concatenate(
        [*terms(tap_side), *terms(forward), np.concatenate(terms(inverse), 1)], 0
    )


def dot(a, b):
    return jnp.dot(a, b, preferred_element_type=jnp.float32)


def column(row):
    return jnp.transpose(jnp.broadcast_to(row, (128, 128)))


def wide(col):
    return jnp.concatenate([col, col], 1)


def sigmoid(value):
    return 0.5 * jnp.tanh(0.5 * value) + 0.5


def lanes(block, size=HALF):
    return pl.ds(pl.multiple_of(block * size, size), size)


def norm_tile(source, cols, gains, layer, store):
    total = jnp.zeros((8, HALF), jnp.float32)
    for r in range(0, 1024, 128):
        piece = source[r : r + 128, cols].astype(jnp.float32)
        square = piece * piece
        for s in range(0, 128, 8):
            total += square[s : s + 8]
    mean = jnp.sum(total, axis=0, keepdims=True) * (1.0 / 1024.0)
    inverse = lax.rsqrt(mean + RMS_EPS)
    for j in range(8):
        r = slice(j * 128, (j + 1) * 128)
        piece = source[r, cols].astype(jnp.float32)
        store[r, :] = (piece * inverse * wide(gains[layer, r])).astype(jnp.bfloat16)


def project_tile(source, tokens, me):
    def product(start):
        r = slice(start, start + 256)
        total = dot(source[r, lanes(me, 512)], tokens[:512])
        total = total + dot(source[r, lanes(1 - me, 512)], tokens[512:])
        return total.astype(jnp.bfloat16).astype(jnp.float32)

    return (product(0) * sigmoid(product(GATE_ROW))).astype(jnp.bfloat16)


def branch(source, layer, half, activated, me):
    r = slice(OUT_ROW + 256 * layer, OUT_ROW + 256 * (layer + 1))
    total = dot(source[r, lanes(2 * half + me)], activated[:256])
    return total + dot(source[r, lanes(2 * half + 1 - me)], activated[256:])


def make_bins(source, layer, part, table):
    lane = (2 * layer + part) * 256
    taps = source[TAP_ROW : TAP_ROW + 128, lane : lane + 256]
    return dot(taps, table[:256]) + dot(taps, table[256:512])


def filter_norm(piece_of, bins, gcols, table, target):
    for chunk in range(2):
        piece = piece_of(slice(chunk * 256, (chunk + 1) * 256))
        freq = dot(piece, table[512:1024]) + dot(piece, table[1024:1536])
        re, im = freq[:, :BINS], freq[:, BINS:]
        tap_re, tap_im = bins[chunk][:, :BINS], bins[chunk][:, BINS:]
        prod = jnp.concatenate([re * tap_re - im * tap_im, re * tap_im + im * tap_re], 1)
        high = prod.astype(jnp.bfloat16)
        low = (prod - high.astype(jnp.float32)).astype(jnp.bfloat16)
        ih, il = table[1536:2048, :KEPT], table[1536:2048, KEPT:]
        filtered = dot(high, ih) + dot(low, ih) + dot(high, il)
        for g in range(2):
            v = filtered[g * 128 : (g + 1) * 128]
            c = slice(chunk * 256 + g * 128, chunk * 256 + (g + 1) * 128)
            centred = v - jnp.mean(v, axis=0, keepdims=True)
            var = jnp.mean(centred * centred, axis=0, keepdims=True)
            scaled = centred * lax.rsqrt(var + LN_EPS)
            scaled = scaled * wide(gcols[0, c]) + wide(gcols[1, c])
            target[c, :] = (scaled * sigmoid(scaled)).astype(jnp.bfloat16)


def group_columns(packs, layer, gcols):
    for chunk, source in enumerate(packs):
        terms = source[GAIN_ROW : GAIN_ROW + 16, :256].astype(jnp.float32)
        for g in range(2):
            for kind in range(2):
                t = terms[:, g * 128 : (g + 1) * 128]
                i = 6 * layer + 3 * kind
                row = t[i : i + 1] + t[i + 1 : i + 2] + t[i + 2 : i + 3]
                start = chunk * 256 + g * 128
                gcols[kind, start : start + 128] = column(row)


def split_kernel(stream, outer, inner):
    me = lax.axis_index("tp")
    outer[...] = stream[:, lanes(me)]
    inner[...] = stream[:, lanes(1 - me)]


def join_kernel(keep, swapped, out):
    me = lax.axis_index("tp")
    other = 1 - me
    out[:, lanes(me)] = keep[...]
    out[:, lanes(other)] = swapped[other]


def early_kernel(gain, pack, table, bins, gains):
    me = lax.axis_index("tp")
    other = 1 - me
    for layer in range(2):
        for half, side in enumerate((me, other)):
            for j in range(4):
                row = gain[layer : layer + 1, lanes(4 * side + j, 128)]
                start = half * 512 + j * 128
                gains[layer, start : start + 128] = column(row)
    for layer in range(2):
        for part in range(2):
            bins[layer, part * 128 : (part + 1) * 128] = make_bins(pack, layer, part, table)


def stored(tile, me):
    return lanes(tile * me + (2 - tile) * (1 - me))


def first_kernel(
    bins, gains, inner, outer, halo_own, halo_other, pack, pack2, table, xw, act,
    normed1, gated, bins2, gcols,
):
    me = lax.axis_index("tp")
    packs = (pack, pack2)

    xw[:512, :256] = inner[...]
    xw[:512, 256:512] = outer[...]
    for tile in range(2):
        start = TOKEN_ROW + 128 * (1 - tile)
        for q in range(4):
            r = slice(512 + 128 * q, 512 + 128 * (q + 1))
            xw[r, 256 * tile : 256 * (tile + 1)] = pack2[
                start : start + 128, 256 * q : 256 * (q + 1)
            ]
    xw[:512, 512:] = halo_own[...]
    xw[512:, 512:] = halo_other[...]
    group_columns(packs, 0, gcols)

    def project_all(tile):
        cols = slice(tile * HALF, (tile + 1) * HALF)
        for chunk, source in enumerate(packs):
            r = slice(chunk * 256, (chunk + 1) * 256)
            gated[r, cols] = project_tile(source, normed1.at[tile], me)

    for tile in range(3):
        norm_tile(xw, slice(tile * HALF, (tile + 1) * HALF), gains, 0, normed1.at[tile])
        if tile:
            project_all(tile - 1)
    for part in range(2):
        bins2[part * 128 : (part + 1) * 128] = make_bins(pack2, 0, part, table)
    project_all(2)

    def piece(b):
        return lambda r: jnp.concatenate([gated[r, stored(b, me)], gated[r, stored(b + 1, me)]], 1)

    own = bins[0], bins2[...]
    for b in range(2):
        filter_norm(piece(b), own, gcols, table, act.at[b])


def second_kernel(
    xw, act, bins, gains, pack, pack2, late, late2, table, keep, send,
    x1, normed2, gated, act2, bins2, gcols,
):
    me = lax.axis_index("tp")
    block = lax.axis_index("sp")

    lane = lax.broadcasted_iota(jnp.int32, (8, KEPT), 1)
    ends = lax.axis_size("sp") - 1
    outside = (
        (lane < FIRST) & ((me == 0) & (block == 0)),
        (lane >= KEPT - FIRST) & ((me == 1) & (block == ends)),
    )

    def finish(b):
        for half, source in enumerate((late, late2)):
            for part in range(2):
                start = half * 512 + part * 256
                r = slice(start, start + 256)
                before = jnp.concatenate(
                    [xw[r, stored(b, me)][:, FIRST:], xw[r, stored(b + 1, me)][:, :FIRST]], 1
                )
                total = before.astype(jnp.float32) + branch(source, 0, part, act[b], me)
                drop = jnp.broadcast_to(outside[b][:1], total.shape)
                total = jnp.where(drop, 0.0, total)
                x1[r, b * KEPT : (b + 1) * KEPT] = total.astype(jnp.bfloat16)

    finish(0)
    norm_tile(x1, slice(0, 256), gains, 1, normed2.at[0])
    finish(1)
    group_columns((pack, pack2), 1, gcols)
    for part in range(2):
        bins2[part * 128 : (part + 1) * 128] = make_bins(pack2, 1, part, table)
    norm_tile(x1, slice(256, 512), gains, 1, normed2.at[1])
    for tile in range(2):
        for chunk, source in enumerate((late, late2)):
            r = slice(chunk * 256, (chunk + 1) * 256)
            cols = slice(tile * HALF, (tile + 1) * HALF)
            gated[r, cols] = project_tile(source, normed2.at[tile], me)
    filter_norm(lambda r: gated[r, :], (bins[1], bins2[...]), gcols, table, act2)
    cols = slice(FIRST, FIRST + KEPT)
    for half, (source, out) in enumerate(((late, keep), (late2, send))):
        for part in range(2):
            start = half * 512 + part * 256
            before = x1[start : start + 256, cols].astype(jnp.float32)
            total = before + branch(source, 1, part, act2, me)
            out[part * 256 : (part + 1) * 256] = total.astype(jnp.bfloat16)


def start_copies(pairs, sems):
    copies = [pltpu.make_async_copy(a, b, sems.at[i]) for i, (a, b) in enumerate(pairs)]
    for copy in copies:
        copy.start()
    return copies


def in_weights(layer, wv, wg, out):
    return [
        (wv.at[layer], out.at[pl.ds(0, 256)]),
        (wg.at[layer], out.at[pl.ds(GATE_ROW, 256)]),
    ]


def pack_kernel(wv, wg, taps0, taps1, ggain, gshift, inner, outer, out, turned, sems):
    copies = start_copies(in_weights(0, wv, wg, out), sems)
    for layer, taps in enumerate((taps0, taps1)):
        count = taps.shape[0]
        turned[:count] = taps[...].astype(jnp.float32)
        turned[count:] = jnp.zeros((256 - count, 256), jnp.float32)
        piece = jnp.transpose(turned[...]).astype(jnp.bfloat16)
        for chunk in range(2):
            lane = (2 * layer + chunk) * 256
            out[TAP_ROW : TAP_ROW + 128, lane : lane + 256] = piece[
                chunk * 128 : (chunk + 1) * 128
            ]
    for half, tokens in enumerate((inner, outer)):
        start = TOKEN_ROW + 128 * half
        for q in range(4):
            out[start : start + 128, 256 * q : 256 * (q + 1)] = tokens[128 * q : 128 * (q + 1)]
    rows = []
    for layer in range(2):
        for source in (ggain, gshift):
            rest = source[layer : layer + 1]
            for _ in range(3):
                term = rest.astype(jnp.bfloat16).astype(jnp.float32)
                rows.append(term)
                rest = rest - term
    rows.append(jnp.zeros((4, 256), jnp.float32))
    rows = jnp.concatenate(rows, 0).astype(jnp.bfloat16)
    out[GAIN_ROW:TOKEN_ROW, :] = jnp.concatenate([rows, rows, rows, rows], 1)
    for copy in copies:
        copy.wait()


def late_pack_kernel(after, wv, wg, wo, out, sems):
    pairs = in_weights(1, wv, wg, out)
    for layer in range(2):
        for part in range(2):
            target = out.at[pl.ds(OUT_ROW + 256 * layer, 256), pl.ds(512 * part, 512)]
            pairs.append((wo.at[layer, pl.ds(256 * part, 256)], target))
    for copy in start_copies(pairs, sems):
        copy.wait()


def call(kernel, arrays, outs, scratch, limit, flops, unread=0, hbm=0):
    vmem = pl.BlockSpec(memory_space=pltpu.VMEM)
    specs = [pl.BlockSpec(memory_space=pl.ANY)] * unread
    specs += [pl.BlockSpec(memory_space=pltpu.HBM)] * hbm
    specs += [vmem] * (len(arrays) - unread - hbm)
    outs = [jax.ShapeDtypeStruct(shape, kind) for shape, kind in outs]
    return pl.pallas_call(
        kernel,
        out_shape=outs,
        in_specs=specs,
        out_specs=[vmem] * len(outs),
        scratch_shapes=scratch,
        compiler_params=pltpu.CompilerParams(vmem_limit_bytes=limit << 20),
        cost_estimate=pl.CostEstimate(
            flops=flops, bytes_accessed=4 * 10**6, transcendentals=2 * 10**5
        ),
    )(*arrays)


def body(blocks, stream, norm_gain, w_value, w_gate, conv_taps, group_gain, group_shift, w_out):
    taps = conv_taps.shape[2]
    both = ("sp", "tp")
    partner = [(i, i ^ 1) for i in range(2 * blocks)]
    outward = [(2 * s + 1, 2 * s + 2) for s in range(blocks - 1)]
    outward += [(2 * s + 2, 2 * s + 1) for s in range(blocks - 1)]
    along = [(2 * s, 2 * s + 2) for s in range(blocks - 1)]
    along += [(2 * s + 3, 2 * s + 1) for s in range(blocks - 1)]

    bf16, f32 = jnp.bfloat16, jnp.float32
    half = ((512, HALF), bf16)
    outer, inner = call(split_kernel, [stream], [half, half], [], 4, 2 * 10**10)
    outer, inner, conv_taps = lax.optimization_barrier((outer, inner, conv_taps))
    tables = jnp.asarray(transform_tables(taps))
    halo_other = lax.ppermute(outer, both, outward)
    halo_own = lax.ppermute(inner, both, along)
    turned = [jnp.transpose(conv_taps[layer]) for layer in range(2)]
    (pack,) = call(
        pack_kernel,
        [w_value, w_gate, *turned, group_gain, group_shift, inner, outer],
        [((PACK_ROWS, 1024), bf16)],
        [pltpu.VMEM((256, 256), f32), pltpu.SemaphoreType.DMA((2,))],
        8, 2 * 10**9, 0, 2,
    )
    pack2 = lax.ppermute(pack, both, partner)
    (late,) = call(
        late_pack_kernel, [pack, w_value, w_gate, w_out],
        [((LATE_ROWS, 1024), bf16)],
        [pltpu.SemaphoreType.DMA((6,))], 4, 10**9, 1, 3,
    )
    late2 = lax.ppermute(late, both, partner)
    bins, gains = call(
        early_kernel,
        [norm_gain, pack, tables],
        [((2, 256, WINDOW), f32), ((2, 1024, 128), f32)],
        [], 12, 10**9,
    )
    xw, act = call(
        first_kernel,
        [bins, gains, inner, outer, halo_own, halo_other, pack, pack2, tables],
        [((1024, 768), bf16), ((2, 512, KEPT), bf16)],
        [
            pltpu.VMEM((3, 1024, HALF), bf16),
            pltpu.VMEM((512, 768), bf16),
            pltpu.VMEM((256, WINDOW), f32),
            pltpu.VMEM((2, 512, 128), f32),
        ],
        16, 4 * 10**9,
    )
    keep, send = call(
        second_kernel,
        [xw, act, bins, gains, pack, pack2, late, late2, tables],
        [((512, KEPT), bf16), ((512, KEPT), bf16)],
        [
            pltpu.VMEM((1024, 512), bf16),
            pltpu.VMEM((2, 1024, HALF), bf16),
            pltpu.VMEM((512, 512), bf16),
            pltpu.VMEM((512, KEPT), bf16),
            pltpu.VMEM((256, WINDOW), f32),
            pltpu.VMEM((2, 512, 128), f32),
        ],
        16, 3 * 10**9,
    )
    swapped = lax.all_gather(send, "tp", axis=0)
    return call(join_kernel, [keep, swapped], [((512, 512), bf16)], [], 4, 10**8)[0]


def solution(mesh):
    placed = (
        P("tp", "sp"),
        P(),
        P(None, "tp", None),
        P(None, "tp", None),
        P(None, "tp", None),
        P(None, "tp"),
        P(None, "tp"),
        P(None, "tp", None),
    )
    return jax.shard_map(
        functools.partial(body, mesh.shape["sp"]),
        mesh=mesh, in_specs=placed, out_specs=P("tp", "sp"), check_vma=False,
    )
```

```python
import functools

import jax
import jax.numpy as jnp
import numpy as np
from jax import lax
from jax.experimental import pallas as pl
from jax.experimental.pallas import tpu as pltpu
from jax.sharding import PartitionSpec as P


RMS_EPS = 1e-06
LN_EPS = 1e-05

WINDOW = 512
KEPT = 256
FIRST = 128
BINS = WINDOW // 2
HALF = 256
GATE_ROW = 256
TAP_ROW = 512
GAIN_ROW = 640
TOKEN_ROW = 656
PACK_ROWS = 912
OUT_ROW = 512
LATE_ROWS = 1024


def transform_tables(taps):
    bins = 2 * np.arange(BINS) + 1
    reach = (taps - 1) // 2

    def angles(left, right):
        return np.pi * (np.outer(left, right) % (2 * WINDOW)) / WINDOW

    time = angles(np.arange(WINDOW), bins)
    lag = angles(np.arange(taps) - reach, bins)
    back = angles(bins, np.arange(FIRST, FIRST + KEPT))
    tap_side = np.concatenate([np.cos(lag), np.sin(lag)], 1) * (2.0 / WINDOW)
    tap_side = np.pad(tap_side, ((0, 256 - taps), (0, 0)))
    forward = np.concatenate([np.cos(time), -np.sin(time)], 1)
    inverse = np.concatenate([np.cos(back), -np.sin(back)], 0)

    def terms(table):
        high = table.astype(jnp.bfloat16)
        return high, (table - high.astype(np.float64)).astype(jnp.bfloat16)

    return np.concatenate(
        [*terms(tap_side), *terms(forward), np.concatenate(terms(inverse), 1)], 0
    )


def dot(a, b):
    return jnp.dot(a, b, preferred_element_type=jnp.float32)


def column(row):
    return jnp.transpose(jnp.broadcast_to(row, (128, 128)))


def wide(col):
    return jnp.concatenate([col, col], 1)


def sigmoid(value):
    return 0.5 * jnp.tanh(0.5 * value) + 0.5


def lanes(block, size=HALF):
    return pl.ds(pl.multiple_of(block * size, size), size)


def norm_tile(source, cols, gains, layer, store):
    total = jnp.zeros((8, HALF), jnp.float32)
    for r in range(0, 1024, 128):
        piece = source[r : r + 128, cols].astype(jnp.float32)
        square = piece * piece
        for s in range(0, 128, 8):
            total += square[s : s + 8]
    mean = jnp.sum(total, axis=0, keepdims=True) * (1.0 / 1024.0)
    inverse = lax.rsqrt(mean + RMS_EPS)
    for j in range(8):
        r = slice(j * 128, (j + 1) * 128)
        piece = source[r, cols].astype(jnp.float32)
        store[r, :] = (piece * inverse * wide(gains[layer, r])).astype(jnp.bfloat16)


def project_tile(source, tokens, me):
    def product(start):
        r = slice(start, start + 256)
        total = dot(source[r, lanes(me, 512)], tokens[:512])
        total = total + dot(source[r, lanes(1 - me, 512)], tokens[512:])
        return total.astype(jnp.bfloat16).astype(jnp.float32)

    return (product(0) * sigmoid(product(GATE_ROW))).astype(jnp.bfloat16)


def branch(source, layer, half, activated, me):
    r = slice(OUT_ROW + 256 * layer, OUT_ROW + 256 * (layer + 1))
    total = dot(source[r, lanes(2 * half + me)], activated[:256])
    return total + dot(source[r, lanes(2 * half + 1 - me)], activated[256:])


def make_bins(source, layer, part, table):
    lane = (2 * layer + part) * 256
    taps = source[TAP_ROW : TAP_ROW + 128, lane : lane + 256]
    return dot(taps, table[:256]) + dot(taps, table[256:512])


def filter_norm(pieces, bins, gcols, table, targets):
    units = [(p, c, t) for p, t in zip(pieces, targets) for c in range(2)]

    def forward(unit):
        piece = unit[0](slice(unit[1] * 256, (unit[1] + 1) * 256))
        return dot(piece, table[512:1024]) + dot(piece, table[1024:1536])

    def spectrum(unit, freq):
        re, im = freq[:, :BINS], freq[:, BINS:]
        tap_re, tap_im = bins[unit[1]][:, :BINS], bins[unit[1]][:, BINS:]
        prod = jnp.concatenate([re * tap_re - im * tap_im, re * tap_im + im * tap_re], 1)
        high = prod.astype(jnp.bfloat16)
        return high, (prod - high.astype(jnp.float32)).astype(jnp.bfloat16)

    def back(high, low):
        ih, il = table[1536:2048, :KEPT], table[1536:2048, KEPT:]
        return dot(high, ih) + dot(low, ih) + dot(high, il)

    def normalize(unit, filtered):
        for g in range(2):
            v = filtered[g * 128 : (g + 1) * 128]
            c = slice(unit[1] * 256 + g * 128, unit[1] * 256 + (g + 1) * 128)
            centred = v - jnp.mean(v, axis=0, keepdims=True)
            var = jnp.mean(centred * centred, axis=0, keepdims=True)
            scaled = centred * lax.rsqrt(var + LN_EPS)
            scaled = scaled * wide(gcols[0, c]) + wide(gcols[1, c])
            unit[2][c, :] = (scaled * sigmoid(scaled)).astype(jnp.bfloat16)

    freq, before = forward(units[0]), None
    for i, unit in enumerate(units):
        following = forward(units[i + 1]) if i + 1 < len(units) else None
        terms = spectrum(unit, freq)
        filtered = back(*terms)
        if before is not None:
            normalize(*before)
        freq, before = following, (unit, filtered)
    normalize(*before)


def group_columns(packs, layer, gcols):
    for chunk, source in enumerate(packs):
        terms = source[GAIN_ROW : GAIN_ROW + 16, :256].astype(jnp.float32)
        for g in range(2):
            for kind in range(2):
                t = terms[:, g * 128 : (g + 1) * 128]
                i = 6 * layer + 3 * kind
                row = t[i : i + 1] + t[i + 1 : i + 2] + t[i + 2 : i + 3]
                start = chunk * 256 + g * 128
                gcols[kind, start : start + 128] = column(row)


def split_kernel(stream, outer, inner):
    me = lax.axis_index("tp")
    outer[...] = stream[:, lanes(me)]
    inner[...] = stream[:, lanes(1 - me)]


def join_kernel(keep, swapped, out):
    me = lax.axis_index("tp")
    other = 1 - me
    out[:, lanes(me)] = keep[...]
    out[:, lanes(other)] = swapped[other]


def early_kernel(gain, pack, table, bins, gains):
    me = lax.axis_index("tp")
    other = 1 - me
    for layer in range(2):
        for half, side in enumerate((me, other)):
            for j in range(4):
                row = gain[layer : layer + 1, lanes(4 * side + j, 128)]
                start = half * 512 + j * 128
                gains[layer, start : start + 128] = column(row)
    for layer in range(2):
        for part in range(2):
            bins[layer, part * 128 : (part + 1) * 128] = make_bins(pack, layer, part, table)


def stored(tile, me):
    return lanes(tile * me + (2 - tile) * (1 - me))


def first_kernel(
    bins, gains, inner, outer, halo_own, halo_other, pack, pack2, table, xw, act,
    normed1, gated, bins2, gcols,
):
    me = lax.axis_index("tp")
    packs = (pack, pack2)

    xw[:512, :256] = inner[...]
    xw[:512, 256:512] = outer[...]
    for tile in range(2):
        start = TOKEN_ROW + 128 * (1 - tile)
        for q in range(4):
            r = slice(512 + 128 * q, 512 + 128 * (q + 1))
            xw[r, 256 * tile : 256 * (tile + 1)] = pack2[
                start : start + 128, 256 * q : 256 * (q + 1)
            ]
    xw[:512, 512:] = halo_own[...]
    xw[512:, 512:] = halo_other[...]
    group_columns(packs, 0, gcols)

    def project_all(tile):
        cols = slice(tile * HALF, (tile + 1) * HALF)
        for chunk, source in enumerate(packs):
            r = slice(chunk * 256, (chunk + 1) * 256)
            gated[r, cols] = project_tile(source, normed1.at[tile], me)

    for tile in range(3):
        norm_tile(xw, slice(tile * HALF, (tile + 1) * HALF), gains, 0, normed1.at[tile])
        if tile:
            project_all(tile - 1)
    for part in range(2):
        bins2[part * 128 : (part + 1) * 128] = make_bins(pack2, 0, part, table)
    project_all(2)

    def piece(b):
        return lambda r: jnp.concatenate([gated[r, stored(b, me)], gated[r, stored(b + 1, me)]], 1)

    own = bins[0], bins2[...]
    filter_norm([piece(0), piece(1)], own, gcols, table, [act.at[0], act.at[1]])


def second_kernel(
    xw, act, bins, gains, pack, pack2, late, late2, table, keep, send,
    x1, normed2, gated, act2, bins2, gcols,
):
    me = lax.axis_index("tp")
    block = lax.axis_index("sp")

    lane = lax.broadcasted_iota(jnp.int32, (8, KEPT), 1)
    ends = lax.axis_size("sp") - 1
    outside = (
        (lane < FIRST) & ((me == 0) & (block == 0)),
        (lane >= KEPT - FIRST) & ((me == 1) & (block == ends)),
    )

    def finish(b):
        for half, source in enumerate((late, late2)):
            for part in range(2):
                start = half * 512 + part * 256
                r = slice(start, start + 256)
                before = jnp.concatenate(
                    [xw[r, stored(b, me)][:, FIRST:], xw[r, stored(b + 1, me)][:, :FIRST]], 1
                )
                total = before.astype(jnp.float32) + branch(source, 0, part, act[b], me)
                drop = jnp.broadcast_to(outside[b][:1], total.shape)
                total = jnp.where(drop, 0.0, total)
                x1[r, b * KEPT : (b + 1) * KEPT] = total.astype(jnp.bfloat16)

    finish(0)
    norm_tile(x1, slice(0, 256), gains, 1, normed2.at[0])
    finish(1)
    group_columns((pack, pack2), 1, gcols)
    for part in range(2):
        bins2[part * 128 : (part + 1) * 128] = make_bins(pack2, 1, part, table)
    norm_tile(x1, slice(256, 512), gains, 1, normed2.at[1])
    for tile in range(2):
        for chunk, source in enumerate((late, late2)):
            r = slice(chunk * 256, (chunk + 1) * 256)
            cols = slice(tile * HALF, (tile + 1) * HALF)
            gated[r, cols] = project_tile(source, normed2.at[tile], me)
    filter_norm([lambda r: gated[r, :]], (bins[1], bins2[...]), gcols, table, [act2])
    cols = slice(FIRST, FIRST + KEPT)
    for half, (source, out) in enumerate(((late, keep), (late2, send))):
        for part in range(2):
            start = half * 512 + part * 256
            before = x1[start : start + 256, cols].astype(jnp.float32)
            total = before + branch(source, 1, part, act2, me)
            out[part * 256 : (part + 1) * 256] = total.astype(jnp.bfloat16)


def start_copies(pairs, sems):
    copies = [pltpu.make_async_copy(a, b, sems.at[i]) for i, (a, b) in enumerate(pairs)]
    for copy in copies:
        copy.start()
    return copies


def in_weights(layer, wv, wg, out):
    return [
        (wv.at[layer], out.at[pl.ds(0, 256)]),
        (wg.at[layer], out.at[pl.ds(GATE_ROW, 256)]),
    ]


def pack_kernel(wv, wg, taps0, taps1, ggain, gshift, inner, outer, out, turned, sems):
    copies = start_copies(in_weights(0, wv, wg, out), sems)
    for layer, taps in enumerate((taps0, taps1)):
        count = taps.shape[0]
        turned[:count] = taps[...].astype(jnp.float32)
        turned[count:] = jnp.zeros((256 - count, 256), jnp.float32)
        piece = jnp.transpose(turned[...]).astype(jnp.bfloat16)
        for chunk in range(2):
            lane = (2 * layer + chunk) * 256
            out[TAP_ROW : TAP_ROW + 128, lane : lane + 256] = piece[
                chunk * 128 : (chunk + 1) * 128
            ]
    for half, tokens in enumerate((inner, outer)):
        start = TOKEN_ROW + 128 * half
        for q in range(4):
            out[start : start + 128, 256 * q : 256 * (q + 1)] = tokens[128 * q : 128 * (q + 1)]
    rows = []
    for layer in range(2):
        for source in (ggain, gshift):
            rest = source[layer : layer + 1]
            for _ in range(3):
                term = rest.astype(jnp.bfloat16).astype(jnp.float32)
                rows.append(term)
                rest = rest - term
    rows.append(jnp.zeros((4, 256), jnp.float32))
    rows = jnp.concatenate(rows, 0).astype(jnp.bfloat16)
    out[GAIN_ROW:TOKEN_ROW, :] = jnp.concatenate([rows, rows, rows, rows], 1)
    for copy in copies:
        copy.wait()


def late_pack_kernel(after, wv, wg, wo, out, sems):
    pairs = in_weights(1, wv, wg, out)
    for layer in range(2):
        for part in range(2):
            target = out.at[pl.ds(OUT_ROW + 256 * layer, 256), pl.ds(512 * part, 512)]
            pairs.append((wo.at[layer, pl.ds(256 * part, 256)], target))
    for copy in start_copies(pairs, sems):
        copy.wait()


def call(kernel, arrays, outs, scratch, limit, flops, unread=0, hbm=0):
    vmem = pl.BlockSpec(memory_space=pltpu.VMEM)
    specs = [pl.BlockSpec(memory_space=pl.ANY)] * unread
    specs += [pl.BlockSpec(memory_space=pltpu.HBM)] * hbm
    specs += [vmem] * (len(arrays) - unread - hbm)
    outs = [jax.ShapeDtypeStruct(shape, kind) for shape, kind in outs]
    return pl.pallas_call(
        kernel,
        out_shape=outs,
        in_specs=specs,
        out_specs=[vmem] * len(outs),
        scratch_shapes=scratch,
        compiler_params=pltpu.CompilerParams(vmem_limit_bytes=limit << 20),
        cost_estimate=pl.CostEstimate(
            flops=flops, bytes_accessed=4 * 10**6, transcendentals=2 * 10**5
        ),
    )(*arrays)


def body(blocks, stream, norm_gain, w_value, w_gate, conv_taps, group_gain, group_shift, w_out):
    taps = conv_taps.shape[2]
    both = ("sp", "tp")
    partner = [(i, i ^ 1) for i in range(2 * blocks)]
    outward = [(2 * s + 1, 2 * s + 2) for s in range(blocks - 1)]
    outward += [(2 * s + 2, 2 * s + 1) for s in range(blocks - 1)]
    along = [(2 * s, 2 * s + 2) for s in range(blocks - 1)]
    along += [(2 * s + 3, 2 * s + 1) for s in range(blocks - 1)]

    bf16, f32 = jnp.bfloat16, jnp.float32
    half = ((512, HALF), bf16)
    outer, inner = call(split_kernel, [stream], [half, half], [], 4, 2 * 10**10)
    outer, inner, conv_taps = lax.optimization_barrier((outer, inner, conv_taps))
    tables = jnp.asarray(transform_tables(taps))
    halo_other = lax.ppermute(outer, both, outward)
    halo_own = lax.ppermute(inner, both, along)
    turned = [jnp.transpose(conv_taps[layer]) for layer in range(2)]
    (pack,) = call(
        pack_kernel,
        [w_value, w_gate, *turned, group_gain, group_shift, inner, outer],
        [((PACK_ROWS, 1024), bf16)],
        [pltpu.VMEM((256, 256), f32), pltpu.SemaphoreType.DMA((2,))],
        8, 2 * 10**9, 0, 2,
    )
    pack2 = lax.ppermute(pack, both, partner)
    (late,) = call(
        late_pack_kernel, [pack, w_value, w_gate, w_out],
        [((LATE_ROWS, 1024), bf16)],
        [pltpu.SemaphoreType.DMA((6,))], 4, 10**9, 1, 3,
    )
    late2 = lax.ppermute(late, both, partner)
    bins, gains = call(
        early_kernel,
        [norm_gain, pack, tables],
        [((2, 256, WINDOW), f32), ((2, 1024, 128), f32)],
        [], 12, 10**9,
    )
    xw, act = call(
        first_kernel,
        [bins, gains, inner, outer, halo_own, halo_other, pack, pack2, tables],
        [((1024, 768), bf16), ((2, 512, KEPT), bf16)],
        [
            pltpu.VMEM((3, 1024, HALF), bf16),
            pltpu.VMEM((512, 768), bf16),
            pltpu.VMEM((256, WINDOW), f32),
            pltpu.VMEM((2, 512, 128), f32),
        ],
        16, 4 * 10**9,
    )
    keep, send = call(
        second_kernel,
        [xw, act, bins, gains, pack, pack2, late, late2, tables],
        [((512, KEPT), bf16), ((512, KEPT), bf16)],
        [
            pltpu.VMEM((1024, 512), bf16),
            pltpu.VMEM((2, 1024, HALF), bf16),
            pltpu.VMEM((512, 512), bf16),
            pltpu.VMEM((512, KEPT), bf16),
            pltpu.VMEM((256, WINDOW), f32),
            pltpu.VMEM((2, 512, 128), f32),
        ],
        16, 3 * 10**9,
    )
    swapped = lax.all_gather(send, "tp", axis=0)
    return call(join_kernel, [keep, swapped], [((512, 512), bf16)], [], 4, 10**8)[0]


def solution(mesh):
    placed = (
        P("tp", "sp"),
        P(),
        P(None, "tp", None),
        P(None, "tp", None),
        P(None, "tp", None),
        P(None, "tp"),
        P(None, "tp"),
        P(None, "tp", None),
    )
    return jax.shard_map(
        functools.partial(body, mesh.shape["sp"]),
        mesh=mesh, in_specs=placed, out_specs=P("tp", "sp"), check_vma=False,
    )
```
